32 devices in a mesh: ep: 16 (over z, y, x), tp: 2 (over core).
Axes of the slice: x: 2, y: 2, z: 4, core: 2. Of those that a mesh axis runs over, the one named last changes fastest.
Arguments:
- tokens: bfloat16 [384, 2048], P('ep'), may hold values from -6 to 6
- attn_gain: float32 [2048], replicated, may hold values from 0.1 to 1.9
- w_query: bfloat16 [2048, 1024], P(None, 'tp'), may hold values from -0.125 to 0.125
- w_key: bfloat16 [2048, 1024], P(None, 'tp'), may hold values from -0.125 to 0.125
- w_value: bfloat16 [2048, 1024], P(None, 'tp'), may hold values from -0.125 to 0.125
- w_zgate: bfloat16 [2048, 1024], P(None, 'tp'), may hold values from -0.125 to 0.125
- w_decay: bfloat16 [2048, 8], P(None, 'tp'), may hold values from -0.125 to 0.125
- w_beta: bfloat16 [2048, 8], P(None, 'tp'), may hold values from -0.125 to 0.125
- decay_rate: float32 [8], P('tp'), may hold values from 0.05 to 2
- decay_bias: float32 [8], P('tp'), may hold values from -3 to 3
- state: float32 [384, 8, 128, 128], P('ep', 'tp'), may hold values from -2 to 2
- out_gain: float32 [128], replicated, may hold values from 0.1 to 1.9
- w_out: bfloat16 [1024, 2048], P('tp'), may hold values from -0.1875 to 0.1875
- ffn_gain: float32 [2048], replicated, may hold values from 0.1 to 1.9
- expert_gate: bfloat16 [16, 2048, 512], P('ep', None, 'tp'), may hold values from -0.125 to 0.125
- expert_up: bfloat16 [16, 2048, 512], P('ep', None, 'tp'), may hold values from -0.125 to 0.125
- expert_down: bfloat16 [16, 512, 2048], P('ep', 'tp'), may hold values from -0.25 to 0.25
- routes: int32 [384, 2], P('ep'), may hold values from 0 to 15, all different within a row; in each aligned block of 24 rows (0 to 23, 24 to 47, ...) at most 6 rows name the same one
- route_weight: float32 [384, 2], P('ep'), may hold values from 0.2 to 1
Outputs:
- layer_out: bfloat16 [384, 2048], P('ep', 'tp')
- new_state: float32 [384, 8, 128, 128], P('ep', 'tp')
The draws below stay inside these ranges and needn't reach their ends.
Inputs may be any that keep to these rules, and one draw needn't show every extreme that they name: `routes`: the 2 entries of a row differ. Among the rows of one index of ep (aligned blocks of 24 rows) no expert is named more than 6 times, a bound that some block reaches.
All inputs are finite; a program needn't handle non-finite values.
Results may differ from the reference program's by a relative error of at most 0.014.
Values may be sent and summed in bfloat16 or wider, within the bound.
A program may use at most 128 MiB of HBM per device.

```python
import math
import jax
import jax.numpy as jnp
import numpy as np
from jax import lax

D = 2048
HEADS = 8
HEAD_DIM = 128
FF_EXP = 512
TOP_K = 2
SEQS_DEV = 24
SEQS = 384
EXPERTS = 16
CAP = 6
N_EP = 16
N_TP = 2


def levels(stream_key, shape, cuts, least, top_value):
    def one(position, blocks):
        draws = jax.random.uniform(jax.random.fold_in(jax.random.fold_in(stream_key, 6), position), (blocks,), jnp.float32, least / len(cuts), top_value / len(cuts))
        return jnp.repeat(jnp.exp(draws), shape[position] // blocks).reshape((-1,) + (1,) * (len(shape) - position - 1))

    factor_of = one(*cuts[0])
    for cut in cuts[1:]:
        factor_of = factor_of * one(*cut)
    return factor_of


def deal_out(rng, own, number, rows, count, top, reach, lean):
    sequence = jax.random.permutation(rng, count)
    heavy_load, ordinary = shares(count, rows * top, reach, lean, True), shares(count, rows * top, reach, lean, False)
    places = jnp.arange(count)

    def named(tallies, rotation):
        used = int((tallies > 0).sum())
        fixed = max(1, used // 4)
        moved = fixed + (places - fixed + rotation * (used - fixed)) % max(1, count - fixed)
        return jnp.zeros((count,), jnp.int32).at[sequence[jnp.where(places < fixed, places, moved)]].set(jnp.asarray(tallies, jnp.int32))

    tallies = jnp.where(number % 4 == 0, named(heavy_load, number // 4), named(ordinary, number - number // 4 - 1))
    mixed = jax.random.permutation(jax.random.fold_in(own, 3), count)
    giver, sink = mixed[0:count // 2 * 2:2], mixed[1:count // 2 * 2:2]
    slack = jnp.minimum(tallies[giver] - 1, reach - tallies[sink]) // 2
    slack = jnp.where((giver == sequence[0]) | (sink == sequence[0]) | (tallies[sink] == 0), 0, jnp.maximum(slack, 0))
    moved = jax.random.randint(jax.random.fold_in(own, 4), (count // 2,), 0, 1 << 20) % (slack + 1)
    tallies = tallies.at[giver].add(-moved).at[sink].add(moved)
    items = jnp.searchsorted(jnp.cumsum(tallies), jnp.arange(rows * top), side="right").astype(jnp.int32)
    listing = items.reshape(top, rows).T
    listing = listing[jax.random.permutation(jax.random.fold_in(own, 1), rows)]
    rotation = jax.random.randint(jax.random.fold_in(own, 2), (rows, 1), 0, top)
    return jnp.take_along_axis(listing, (jnp.arange(top)[None, :] + rotation) % top, axis=1)


def shares(amount, total, reach, slope, full):
    weights = [(1 << 20) // math.isqrt(rank ** slope) + 1 for rank in range(1, amount + 1)]
    largest = reach if full else min(reach, max(-(-total // amount), total * weights[0] // sum(weights)))
    least = 1 if total - largest >= amount - 1 else 0
    counts, rest = [largest] + [least] * (amount - 1), total - largest - least * (amount - 1)
    while rest > 0:
        movable = [i for i in range(1, amount) if counts[i] < largest] or [i for i in range(1, amount) if counts[i] < reach]
        pool, budget = sum([weights[i] for i in movable]), rest
        for i in movable:
            extra = min(reach - counts[i], max(1, budget * weights[i] // pool), rest)
            counts[i] = counts[i] + extra
            rest = rest - extra
    return np.array(counts)


def normal_values(stream_key, dims, width, limit, shards=(), kind=jnp.bfloat16):
    entries = width * jax.random.normal(stream_key, dims, jnp.float32)
    if shards:
        entries = entries * levels(stream_key, dims, shards, -0.22, 0.18)
    return jnp.clip(entries, -limit, limit).astype(kind)


def setup_inputs(seed: int = 0) -> dict:
    streams_of = jax.random.split(jax.random.key(seed), 20)
    tokens = normal_values(streams_of[0], (SEQS, D), 1.0, 6.0, ((0, 16),))
    attn_gain = jnp.clip(1.0 + 0.18 * jax.random.normal(streams_of[1], (D,), jnp.float32), 0.1, 1.9)
    w_query = normal_values(streams_of[2], (D, HEADS * HEAD_DIM), D ** -0.5, 0.125, ((1, 2),))
    w_key = normal_values(streams_of[3], (D, HEADS * HEAD_DIM), D ** -0.5, 0.125, ((1, 2),))
    w_value = normal_values(streams_of[4], (D, HEADS * HEAD_DIM), D ** -0.5, 0.125, ((1, 2),))
    w_zgate = normal_values(streams_of[5], (D, HEADS * HEAD_DIM), D ** -0.5, 0.125, ((1, 2),))
    w_decay = normal_values(streams_of[6], (D, HEADS), D ** -0.5, 0.125, ((1, 2),))
    w_beta = normal_values(streams_of[7], (D, HEADS), D ** -0.5, 0.125, ((1, 2),))
    decay_rate = jnp.clip(jnp.exp(math.log(2.0) - 3.6888794 * jax.random.uniform(streams_of[8], (HEADS,), jnp.float32) ** levels(streams_of[8], (HEADS,), ((0, 2),), -0.2, 0.2)), 0.05, 2.0)
    decay_bias = normal_values(streams_of[9], (HEADS,), 1.0, 3.0, ((0, 2),), jnp.float32)
    state = normal_values(streams_of[10], (SEQS, HEADS, HEAD_DIM, HEAD_DIM), 0.3, 2.0, ((0, 16), (1, 2)), jnp.float32)
    out_gain = jnp.clip(1.0 + 0.18 * jax.random.normal(streams_of[11], (HEAD_DIM,), jnp.float32), 0.1, 1.9)
    w_out = normal_values(streams_of[12], (HEADS * HEAD_DIM, D), (HEADS * HEAD_DIM) ** -0.5, 0.1875, ((0, 2),))
    ffn_gain = jnp.clip(1.0 + 0.18 * jax.random.normal(streams_of[13], (D,), jnp.float32), 0.1, 1.9)
    expert_gate = normal_values(streams_of[14], (EXPERTS, D, FF_EXP), D ** -0.5, 0.125, ((0, 16), (2, 2)))
    expert_up = normal_values(streams_of[15], (EXPERTS, D, FF_EXP), D ** -0.5, 0.125, ((0, 16), (2, 2)))
    expert_down = normal_values(streams_of[16], (EXPERTS, FF_EXP, D), FF_EXP ** -0.5, 0.25, ((0, 16), (1, 2)))
    routes_keys = jax.random.split(jax.random.fold_in(streams_of[17], 1), SEQS // SEQS_DEV)
    routes_turns = jax.random.permutation(jax.random.fold_in(streams_of[17], 3), SEQS // SEQS_DEV)
    routes = jax.vmap(lambda own, number: deal_out(jax.random.fold_in(streams_of[17], 2), own, number, SEQS_DEV, EXPERTS, TOP_K, CAP, 2))(routes_keys, routes_turns).reshape((SEQS, TOP_K))
    route_weight = jnp.clip(0.2 + 0.8 * jax.random.uniform(streams_of[18], (SEQS, TOP_K), jnp.float32) ** levels(streams_of[18], (SEQS, TOP_K), ((0, 16),), -0.2, 0.2), 0.2, 1.0)
    return dict(tokens=tokens, attn_gain=attn_gain, w_query=w_query, w_key=w_key, w_value=w_value, w_zgate=w_zgate, w_decay=w_decay, w_beta=w_beta, decay_rate=decay_rate, decay_bias=decay_bias, state=state, out_gain=out_gain, w_out=w_out, ffn_gain=ffn_gain, expert_gate=expert_gate, expert_up=expert_up, expert_down=expert_down, routes=routes, route_weight=route_weight)


EPS = 1e-06

def rms_scale(rows, gain):
    return rows * lax.rsqrt(lax.optimization_barrier(jnp.mean(rows * rows, axis=-1, keepdims=True)) + EPS) * gain

def unit_rows(rows):
    return rows * lax.rsqrt(lax.optimization_barrier(jnp.sum(rows * rows, axis=-1, keepdims=True)) + EPS)

def mixer_block(args):
    normed, w_query, w_key, w_value, w_zgate, w_decay, w_beta, decay_rate, decay_bias, state, out_gain = args
    seqs = normed.shape[0]

    def project(weight):
        return jnp.dot(normed, weight, preferred_element_type=jnp.float32).astype(jnp.bfloat16)

    def heads_of(raw):
        return raw.reshape(seqs, HEADS, HEAD_DIM).astype(jnp.float32)
    query = unit_rows(jax.nn.silu(heads_of(project(w_query)))) * HEAD_DIM ** (-0.5)
    key = unit_rows(jax.nn.silu(heads_of(project(w_key))))
    value = jax.nn.silu(heads_of(project(w_value)))
    zmul = jax.nn.silu(heads_of(project(w_zgate)))
    fade = jnp.exp(-decay_rate * jax.nn.softplus(project(w_decay).astype(jnp.float32) + decay_bias))
    beta = jax.nn.sigmoid(project(w_beta).astype(jnp.float32))
    predicted = jnp.einsum('shkv,shk->shv', state, key, precision=lax.Precision.HIGHEST)
    written = beta[..., None] * (value - fade[..., None] * predicted)
    updated = fade[..., None, None] * state + key[..., :, None] * written[..., None, :]
    read = jnp.einsum('shkv,shk->shv', updated, query, precision=lax.Precision.HIGHEST)
    heads_out = (rms_scale(read, out_gain) * zmul).astype(jnp.bfloat16)
    return (heads_out.reshape(seqs, HEADS * HEAD_DIM), updated)

def reference(tokens, attn_gain, w_query, w_key, w_value, w_zgate, w_decay, w_beta, decay_rate, decay_bias, state, out_gain, w_out, ffn_gain, expert_gate, expert_up, expert_down, routes, route_weight):
    resid_in = tokens.astype(jnp.float32)
    normed = rms_scale(resid_in, attn_gain).astype(jnp.bfloat16)

    def one_block(args):
        block_rows, block_state = args
        return mixer_block((block_rows, w_query, w_key, w_value, w_zgate, w_decay, w_beta, decay_rate, decay_bias, block_state, out_gain))
    heads_out, new_state = lax.map(one_block, (normed.reshape(N_EP, SEQS_DEV, D), state.reshape(N_EP, SEQS_DEV, HEADS, HEAD_DIM, HEAD_DIM)))
    heads_out = heads_out.reshape(SEQS, HEADS * HEAD_DIM)
    new_state = new_state.reshape(SEQS, HEADS, HEAD_DIM, HEAD_DIM)
    group = HEADS * HEAD_DIM // N_TP
    mixed = jnp.zeros((SEQS, D), jnp.float32)
    for part in range(N_TP):
        term = jnp.dot(heads_out[:, part * group:(part + 1) * group], w_out[part * group:(part + 1) * group], preferred_element_type=jnp.float32)
        mixed = mixed + term.astype(jnp.bfloat16).astype(jnp.float32)
    resid = resid_in + mixed
    moe_in = rms_scale(resid, ffn_gain).astype(jnp.bfloat16)
    flat = routes.reshape(N_EP, SEQS_DEV * TOP_K)
    onehot = (flat[..., None] == jnp.arange(EXPERTS, dtype=jnp.int32)[None, None, :]).astype(jnp.int32)
    before = jnp.cumsum(onehot, axis=1) - onehot
    slot = lax.optimization_barrier(jnp.sum(before * onehot, axis=-1)).astype(jnp.int32)
    block_ids = jnp.broadcast_to(jnp.arange(N_EP, dtype=jnp.int32)[:, None], flat.shape)
    row_of = (jnp.arange(SEQS_DEV * TOP_K, dtype=jnp.int32) // TOP_K)[None, :] + SEQS_DEV * block_ids
    table = jnp.zeros((EXPERTS, N_EP, CAP), jnp.int32).at[flat, block_ids, slot].set(row_of.astype(jnp.int32))
    piece = FF_EXP // N_TP

    def run_expert(args):
        w_gate, w_up, w_down, picks = args
        rows = moe_in[picks.reshape(-1)]
        gate = jnp.dot(rows, w_gate, preferred_element_type=jnp.float32)
        up = jnp.dot(rows, w_up, preferred_element_type=jnp.float32)
        hidden = (jax.nn.silu(gate) * up).astype(jnp.bfloat16)
        total = jnp.zeros((rows.shape[0], D), jnp.float32)
        for part in range(N_TP):
            term = jnp.dot(hidden[:, part * piece:(part + 1) * piece], w_down[part * piece:(part + 1) * piece], preferred_element_type=jnp.float32)
            total = total + term.astype(jnp.bfloat16).astype(jnp.float32)
        return total.astype(jnp.bfloat16).reshape(N_EP, CAP, D)
    results = lax.map(run_expert, (expert_gate, expert_up, expert_down, table))
    per_route = results[flat, block_ids, slot].astype(jnp.float32).reshape(SEQS, TOP_K, D)
    combined = lax.optimization_barrier(jnp.sum(per_route * route_weight[..., None], axis=1))
    layer_out = (resid + combined).astype(jnp.bfloat16)
    return (layer_out, new_state)
```

```python
import functools

import jax
import jax.numpy as jnp
from jax import lax
from jax.experimental import pallas as pl
from jax.experimental.pallas import tpu as pltpu
from jax.sharding import PartitionSpec as P

EPS = 1e-06
F32 = jnp.float32
BF16 = jnp.bfloat16
VMEM_LIMIT = 44 * 1024 * 1024
HBM = pl.BlockSpec(memory_space=pltpu.HBM)
VMEM = pl.BlockSpec(memory_space=pltpu.VMEM)


def rms_scale(rows, gain):
    return rows * lax.rsqrt(jnp.mean(rows * rows, axis=-1, keepdims=True) + EPS) * gain


def unit_rows(rows):
    return rows * lax.rsqrt(jnp.sum(rows * rows, axis=-1, keepdims=True) + EPS)


def silu(x):
    return x * jax.nn.sigmoid(x)


def nt_dot(rows, weight):
    return lax.dot_general(rows, weight, (((1,), (1,)), ((), ())), preferred_element_type=F32)


def iota(shape, axis):
    return lax.broadcasted_iota(jnp.int32, shape, axis)


def layer_kernel(
    n_ep,
    n_tp,
    top,
    cap,
    shares,
    step,
    tokens_ref,
    attn_ref,
    wd_ref,
    wb_ref,
    rate_ref,
    bias_ref,
    og_ref,
    ffn_ref,
    routes_ref,
    weights_ref,
    wq,
    wk,
    wv,
    wz,
    state,
    w_out,
    w_gate,
    w_up,
    w_down,
    out,
    ns,
    tokens,
    attn_gain,
    wd,
    wb,
    rate,
    bias,
    out_gain,
    ffn_gain,
    routes,
    weights,
    wbuf,
    wo,
    wg,
    wu,
    wdn,
    kq,
    vals,
    zbuf,
    fades,
    betas,
    dots,
    reads,
    spread,
    picks,
    part_out,
    part_in,
    resid,
    disp,
    arrived,
    ret_out,
    ret_in,
    small_sem,
    w_sem,
    in_sem,
    x_sem,
    part_sem,
    push_sem,
    go_sem,
    back_sem,
    back_recv,
):
    seqs, heads, dim, _ = ns.shape
    width = tokens.shape[1]
    cols = width // n_tp
    chunks = seqs // step
    e = lax.axis_index("ep")
    t = lax.axis_index("tp")
    u = n_tp - 1 - t
    mesh_ids = pl.DeviceIdType.MESH
    partner = {"ep": e, "tp": u}
    barrier = pltpu.get_barrier_semaphore()
    pl.semaphore_signal(barrier, inc=1, device_id=partner, device_id_type=mesh_ids)

    def far(i):
        k = (i + 1) // 2
        return lax.rem(e + n_ep // 2 + k * (2 * lax.rem(i, 2) - 1) + n_ep, n_ep)

    def greet(i, carry):
        pl.semaphore_signal(barrier, inc=1, device_id={"ep": far(i), "tp": t}, device_id_type=mesh_ids)
        return carry

    lax.fori_loop(0, n_ep - 1, greet, 0)

    def in_copy(c):
        rows = pl.ds(c * step, step)
        return pltpu.make_async_copy(state.at[rows], ns.at[rows], in_sem.at[c])

    small = [
        pltpu.make_async_copy(src, dst, small_sem.at[n])
        for n, (src, dst) in enumerate(
            (
                (tokens_ref, tokens),
                (attn_ref, attn_gain),
                (wd_ref, wd),
                (wb_ref, wb),
                (rate_ref, rate),
                (bias_ref, bias),
                (og_ref, out_gain),
                (ffn_ref, ffn_gain),
                (routes_ref, routes),
                (weights_ref, weights),
            )
        )
    ]
    load = [pltpu.make_async_copy(src, wbuf.at[n], w_sem.at[n]) for n, src in enumerate((wq, wk, wv, wz))]
    load.append(pltpu.make_async_copy(w_out, wo, w_sem.at[4]))
    experts = [
        pltpu.make_async_copy(src.at[0], dst.at[t], x_sem.at[n])
        for n, (src, dst) in enumerate(((w_gate, wg), (w_up, wu), (w_down, wdn)))
    ]
    push = [
        pltpu.make_async_remote_copy(
            src_ref=dst.at[t],
            dst_ref=dst.at[t],
            send_sem=push_sem.at[0, n],
            recv_sem=push_sem.at[1, n],
            device_id=partner,
            device_id_type=mesh_ids,
        )
        for n, dst in enumerate((wg, wu, wdn))
    ]
    for copy in small:
        copy.start()
    for n in range(3):
        load[n].start()
    for copy in small:
        copy.wait()
    lax.fori_loop(0, chunks, lambda c, carry: (in_copy(c).start(), carry)[1], 0)

    normed = rms_scale(tokens[...].astype(F32), attn_gain[...]).astype(BF16)

    def rounded(weight):
        return jnp.dot(normed, weight, preferred_element_type=F32).astype(BF16).astype(F32)

    xa = nt_dot(normed, wd[...]).astype(BF16).astype(F32) + bias[...]
    fade = jnp.exp(-rate[...] * (jnp.maximum(xa, 0.0) + jnp.log1p(jnp.exp(-jnp.abs(xa)))))
    beta = jax.nn.sigmoid(nt_dot(normed, wb[...]).astype(BF16).astype(F32))
    for h in range(heads):
        fades[:, h, :] = jnp.broadcast_to(fade[:, h : h + 1], (seqs, dim))
        betas[:, h, :] = jnp.broadcast_to(beta[:, h : h + 1], (seqs, dim))

    eye = iota((seqs, seqs), 1) == iota((seqs, seqs), 0)

    def column(row):
        return jnp.sum(jnp.where(eye, row, 0.0), axis=1, keepdims=True)

    lower = (iota((seqs, seqs), 1) < iota((seqs, seqs), 0)).astype(BF16)
    slots = n_ep * cap
    taken = jnp.zeros((1, n_ep), F32)
    found = []
    mine = jnp.zeros((seqs, slots), F32)
    for j in range(top):
        route = column(routes[j : j + 1, :].astype(F32)).astype(jnp.int32)
        hot = (iota((seqs, n_ep), 1) == route).astype(F32)
        before = jnp.dot(lower, hot.astype(BF16), preferred_element_type=F32) + taken
        slot = jnp.sum(before * hot, axis=1, keepdims=True).astype(jnp.int32)
        taken = taken + jnp.sum(hot, axis=0, keepdims=True)
        place = route * cap + slot + jnp.where(slot < shares[0], 0, slots - shares[0])
        found.append((iota((seqs, n_tp * slots), 1) == place).astype(F32))
        mine = mine + (iota((seqs, slots), 1) + t * slots == place).astype(F32)
    spread[...] = mine.T.astype(BF16)
    picks[...] = jnp.concatenate(found, axis=0).astype(BF16)

    load[0].wait()
    raw_q = rounded(wbuf[0])
    load[1].wait()
    raw_k = rounded(wbuf[1])
    for n in (3, 4):
        load[n].start()
    for h in range(heads):
        span = slice(h * dim, (h + 1) * dim)
        query = unit_rows(silu(raw_q[:, span])) * dim ** (-0.5)
        key = unit_rows(silu(raw_k[:, span]))
        kq[:, h, :] = key
        kq[:, heads + h, :] = query
        dots[:, h, :] = jnp.broadcast_to(jnp.sum(key * query, axis=-1, keepdims=True), (seqs, dim))
    load[2].wait()
    value = silu(rounded(wbuf[2]))
    for h in range(heads):
        vals[:, h, :] = value[:, h * dim : (h + 1) * dim]
    for copy in experts:
        copy.start()

    def one_chunk(c, carry):
        in_copy(c).wait()
        hits = []
        for i in range(step):
            s = c * step + i
            lhs = kq[s].astype(BF16)
            hits.append([jnp.dot(lhs, ns[s, h].astype(BF16), preferred_element_type=F32) for h in range(heads)])
        for i in range(step):
            s = c * step + i
            turned = kq[s].T
            fs, bs, vs, ds = fades[s], betas[s], vals[s], dots[s]
            for h in range(heads):
                hit = hits[i][h]
                f = fs[h : h + 1]
                written = bs[h : h + 1] * (vs[h : h + 1] - f * hit[h : h + 1])
                kc = jnp.broadcast_to(turned[:, h : h + 1], (dim, dim))
                ns[s, h] = f * ns[s, h] + kc * written
                reads[s, pl.ds(h, 1)] = f * hit[heads + h : heads + h + 1] + written * ds[h : h + 1]
        return carry

    lax.fori_loop(0, chunks, one_chunk, 0)
    load[3].wait()
    zbuf[...] = silu(rounded(wbuf[3]))
    mixed = []
    for h in range(heads):
        span = slice(h * dim, (h + 1) * dim)
        mixed.append((rms_scale(reads[:, h, :], out_gain[...]) * zbuf[:, span]).astype(BF16))
    load[4].wait()
    part_out[...] = jnp.dot(jnp.concatenate(mixed, axis=1), wo[...], preferred_element_type=F32).astype(BF16)
    pl.semaphore_wait(barrier, n_ep)

    swap = pltpu.make_async_remote_copy(
        src_ref=part_out,
        dst_ref=part_in,
        send_sem=part_sem.at[0],
        recv_sem=part_sem.at[1],
        device_id=partner,
        device_id_type=mesh_ids,
    )
    swap.start()
    experts[0].wait()
    push[0].start()
    swap.wait()
    rows = tokens[...].astype(F32) + (part_out[...].astype(F32) + part_in[...].astype(F32))
    resid[...] = rows
    moe = rms_scale(rows, ffn_gain[...]).astype(BF16)
    going = jnp.dot(spread[...], moe, preferred_element_type=F32)
    disp[...] = going.reshape(n_ep, cap, width).astype(BF16)

    def go(n, p):
        return pltpu.make_async_remote_copy(
            src_ref=disp.at[p, pl.ds(0, n)],
            dst_ref=arrived.at[e, pl.ds(0, n)],
            send_sem=go_sem.at[0],
            recv_sem=go_sem.at[1],
            device_id={"ep": p, "tp": t},
            device_id_type=mesh_ids,
        )

    def all_go(n, which):
        block = arrived.at[pl.ds(0, n_ep - 1), pl.ds(0, n)]
        return pltpu.make_async_copy(block, block, go_sem.at[which])

    def back(n, c, p):
        return pltpu.make_async_remote_copy(
            src_ref=ret_out.at[c, p, pl.ds(0, n)],
            dst_ref=ret_in.at[t, e, pl.ds(0, n)],
            send_sem=back_sem.at[0],
            recv_sem=back_recv.at[t],
            device_id={"ep": p, "tp": c},
            device_id_type=mesh_ids,
        )

    def all_back(n, c, count, sem):
        block = ret_in.at[c, pl.ds(0, count), pl.ds(0, n)]
        return pltpu.make_async_copy(block, block, sem)

    for c, n in enumerate(shares):
        if n:

            @pl.when(t == c)
            def _(n=n):
                lax.fori_loop(0, n_ep - 1, lambda i, carry: (go(n, far(i)).start(), carry)[1], 0)

    arrived[e] = disp[e]
    for n in (1, 2):
        experts[n].wait()
        push[n].start()
    for c, n in enumerate(shares):
        if n:

            @pl.when(t == c)
            def _(n=n):
                all_go(n, 1).wait()

    got = arrived[...].astype(F32).reshape(slots, width).astype(BF16)
    push[0].wait_recv()
    gates = [jnp.dot(got, wg[h], preferred_element_type=F32) for h in range(n_tp)]
    push[1].wait_recv()
    ups = [jnp.dot(got, wu[h], preferred_element_type=F32) for h in range(n_tp)]
    hidden = [(silu(gates[h]) * ups[h]).astype(BF16) for h in range(n_tp)]
    push[2].wait_recv()
    for c in range(n_tp):
        term = None
        for h in range(n_tp):
            piece = jnp.dot(hidden[h], wdn[h, :, c * cols : (c + 1) * cols], preferred_element_type=F32)
            term = piece if term is None else term + piece
        ret_out[c] = term.reshape(n_ep, cap, cols).astype(BF16)

    for c, n in enumerate(shares):
        if n:

            @pl.when(t == c)
            def _(n=n, c=c):
                def send(i, carry):
                    for d in range(n_tp):
                        back(n, d, far(i)).start()
                    return carry

                lax.fori_loop(0, n_ep - 1, send, 0)
                for d in range(n_tp):
                    if d != c:
                        back(n, d, e).start()

    ret_in[t, e] = ret_out[t, e]
    total = resid[:, pl.ds(pl.multiple_of(t * cols, 128), cols)]
    scale = [column(weights[j : j + 1, :]) for j in range(top)]
    for c, n in enumerate(shares):
        if n:
            for d in range(n_tp):

                @pl.when(t == d)
                def _(n=n, c=c, d=d):
                    all_back(n, c, n_ep - (c == d), back_recv.at[c]).wait()

    kept = [(iota((n_ep, cap, cols), 1) < n) for n in shares]
    returned = [
        jnp.where(kept[c], ret_in[c].astype(F32), 0.0).reshape(slots, cols).astype(BF16) for c in range(n_tp)
    ]
    combined = jnp.dot(picks[...], jnp.concatenate(returned, axis=0), preferred_element_type=F32)
    for j in range(top):
        total = total + combined[j * seqs : (j + 1) * seqs] * scale[j]
    out[...] = total.astype(BF16)

    for copy in push:
        copy.wait_send()
    for c, n in enumerate(shares):
        if n:

            @pl.when(t == c)
            def _(n=n):
                all_go(n, 0).wait()
                for d in range(n_tp):
                    all_back(n, d, n_ep - 1 + d, back_sem.at[0]).wait()


def per_device(
    n_ep,
    n_tp,
    tokens,
    attn_gain,
    w_query,
    w_key,
    w_value,
    w_zgate,
    w_decay,
    w_beta,
    decay_rate,
    decay_bias,
    state,
    out_gain,
    w_out,
    ffn_gain,
    expert_gate,
    expert_up,
    expert_down,
    routes,
    route_weight,
):
    seqs, width = tokens.shape
    heads, dim = state.shape[1], state.shape[2]
    top = routes.shape[1]
    inner = heads * dim
    step = 4 if seqs % 4 == 0 else 1
    chunks = seqs // step
    live = max(2, 2 * seqs * top // n_ep)
    first = 2 * -(-live // 4)
    shares = (first, live - first)
    cap = -(-first // 8) * 8
    cols = width // n_tp
    ff = expert_gate.shape[2]
    slots = n_ep * cap
    vmem = pltpu.VMEM
    dma = pltpu.SemaphoreType.DMA
    return pl.pallas_call(
        functools.partial(layer_kernel, n_ep, n_tp, top, cap, shares, step),
        out_shape=(vmem((seqs, cols), BF16), vmem(state.shape, F32)),
        in_specs=[HBM] * 19,
        out_specs=(VMEM, VMEM),
        scratch_shapes=[
            vmem((seqs, width), BF16),
            vmem((1, width), F32),
            vmem((heads, width), BF16),
            vmem((heads, width), BF16),
            vmem((1, heads), F32),
            vmem((1, heads), F32),
            vmem((1, dim), F32),
            vmem((1, width), F32),
            vmem((top, seqs), jnp.int32),
            vmem((top, seqs), F32),
            vmem((4, width, inner), BF16),
            vmem((inner, width), BF16),
            vmem((n_tp, width, ff), BF16),
            vmem((n_tp, width, ff), BF16),
            vmem((n_tp, ff, width), BF16),
            vmem((seqs, 2 * heads, dim), F32),
            vmem((seqs, heads, dim), F32),
            vmem((seqs, inner), F32),
            vmem((seqs, heads, dim), F32),
            vmem((seqs, heads, dim), F32),
            vmem((seqs, heads, dim), F32),
            vmem((seqs, heads, dim), F32),
            vmem((slots, seqs), BF16),
            vmem((top * seqs, n_tp * slots), BF16),
            vmem((seqs, width), BF16),
            vmem((seqs, width), BF16),
            vmem((seqs, width), F32),
            vmem((n_ep, cap, width), BF16),
            vmem((n_ep, cap, width), BF16),
            vmem((n_tp, n_ep, cap, cols), BF16),
            vmem((n_tp, n_ep, cap, cols), BF16),
            dma((10,)),
            dma((5,)),
            dma((chunks,)),
            dma((3,)),
            dma((2,)),
            dma((2, 3)),
            dma((2,)),
            dma((1,)),
            dma((n_tp,)),
        ],
        compiler_params=pltpu.CompilerParams(
            collective_id=0, has_side_effects=True, vmem_limit_bytes=VMEM_LIMIT
        ),
        name="layer",
    )(
        tokens,
        attn_gain.reshape(1, width),
        w_decay.T,
        w_beta.T,
        decay_rate.reshape(1, heads),
        decay_bias.reshape(1, heads),
        out_gain.reshape(1, dim),
        ffn_gain.reshape(1, width),
        routes.T,
        route_weight.T,
        w_query,
        w_key,
        w_value,
        w_zgate,
        state,
        w_out,
        expert_gate,
        expert_up,
        expert_down,
    )


def solution(mesh):
    in_specs = (
        P("ep", None),
        P(),
        P(None, "tp"),
        P(None, "tp"),
        P(None, "tp"),
        P(None, "tp"),
        P(None, "tp"),
        P(None, "tp"),
        P("tp"),
        P("tp"),
        P("ep", "tp", None, None),
        P(),
        P("tp", None),
        P(),
        P("ep", None, "tp"),
        P("ep", None, "tp"),
        P("ep", "tp", None),
        P("ep", None),
        P("ep", None),
    )
    out_specs = (P("ep", "tp"), P("ep", "tp", None, None))
    body = functools.partial(per_device, mesh.shape["ep"], mesh.shape["tp"])
    return jax.shard_map(body, mesh=mesh, in_specs=in_specs, out_specs=out_specs, check_vma=False)
```

```python
import functools

import jax
import jax.numpy as jnp
from jax import lax
from jax.experimental import pallas as pl
from jax.experimental.pallas import tpu as pltpu
from jax.sharding import PartitionSpec as P

EPS = 1e-06
F32 = jnp.float32
BF16 = jnp.bfloat16
VMEM_LIMIT = 57 * 1024 * 1024
HBM = pl.BlockSpec(memory_space=pltpu.HBM)
VMEM = pl.BlockSpec(memory_space=pltpu.VMEM)


def rms_scale(rows, gain):
    return rows * lax.rsqrt(jnp.mean(rows * rows, axis=-1, keepdims=True) + EPS) * gain


def unit_rows(rows):
    return rows * lax.rsqrt(jnp.sum(rows * rows, axis=-1, keepdims=True) + EPS)


def silu(x):
    return x * jax.nn.sigmoid(x)


def nt_dot(rows, weight):
    return lax.dot_general(rows, weight, (((1,), (1,)), ((), ())), preferred_element_type=F32)


def iota(shape, axis):
    return lax.broadcasted_iota(jnp.int32, shape, axis)


def layer_kernel(
    n_ep,
    n_tp,
    top,
    cap,
    shares,
    step,
    tokens_ref,
    attn_ref,
    wd_ref,
    wb_ref,
    rate_ref,
    bias_ref,
    og_ref,
    ffn_ref,
    routes_ref,
    weights_ref,
    wq,
    wk,
    wv,
    wz,
    state,
    w_out,
    w_gate,
    w_up,
    w_down,
    out,
    ns,
    tokens,
    attn_gain,
    wd,
    wb,
    rate,
    bias,
    out_gain,
    ffn_gain,
    routes,
    weights,
    wbuf,
    wo,
    wg,
    wu,
    wdn,
    kq,
    vals,
    zbuf,
    fades,
    betas,
    dots,
    turned,
    reads,
    spread,
    picks,
    part_out,
    part_in,
    resid,
    disp,
    arrived,
    ret_out,
    ret_in,
    small_sem,
    w_sem,
    in_sem,
    x_sem,
    part_sem,
    push_sem,
    go_sem,
    back_sem,
    back_recv,
):
    seqs, heads, dim, _ = ns.shape
    width = tokens.shape[1]
    cols = width // n_tp
    chunks = seqs // step
    e = lax.axis_index("ep")
    t = lax.axis_index("tp")
    u = n_tp - 1 - t
    mesh_ids = pl.DeviceIdType.MESH
    partner = {"ep": e, "tp": u}
    barrier = pltpu.get_barrier_semaphore()
    pl.semaphore_signal(barrier, inc=1, device_id=partner, device_id_type=mesh_ids)

    bits = [1 << b for b in range((n_ep - 1).bit_length())] if n_ep & (n_ep - 1) == 0 else []
    flips = [bit * (1 - 2 * lax.rem(e // bit, 2)) for bit in bits]

    def across(i):
        if not bits:
            return lax.rem(e + 1 + i, n_ep)
        p = e
        for bit, flip in zip(bits, flips):
            p = p + flip * lax.rem((n_ep - 1 - i) // bit, 2)
        return p

    def rising(i):
        return lax.rem(i + jnp.where(i >= e, 1, 0), n_ep)

    def greet(i, carry):
        pl.semaphore_signal(barrier, inc=1, device_id={"ep": rising(i), "tp": t}, device_id_type=mesh_ids)
        return carry

    lax.fori_loop(0, n_ep - 1, greet, 0)

    def in_copy(c):
        rows = pl.ds(c * step, step)
        return pltpu.make_async_copy(state.at[rows], ns.at[rows], in_sem.at[c])

    small = [
        pltpu.make_async_copy(src, dst, small_sem.at[n])
        for n, (src, dst) in enumerate(
            (
                (tokens_ref, tokens),
                (attn_ref, attn_gain),
                (wd_ref, wd),
                (wb_ref, wb),
                (rate_ref, rate),
                (bias_ref, bias),
                (og_ref, out_gain),
                (ffn_ref, ffn_gain),
                (routes_ref, routes),
                (weights_ref, weights),
            )
        )
    ]
    weight = [(src, wbuf.at[n]) for n, src in enumerate((wq, wk, wv, wz))] + [(w_out, wo)]

    def load_start(n):
        pltpu.make_async_copy(*weight[n], w_sem.at[n]).start()

    def load_wait(n):
        pltpu.make_async_copy(*weight[n], w_sem.at[n]).wait()

    experts = [
        pltpu.make_async_copy(src.at[0], dst.at[t], x_sem.at[n])
        for n, (src, dst) in enumerate(((w_gate, wg), (w_up, wu), (w_down, wdn)))
    ]
    push = [
        pltpu.make_async_remote_copy(
            src_ref=dst.at[t],
            dst_ref=dst.at[t],
            send_sem=push_sem.at[0, n],
            recv_sem=push_sem.at[1, n],
            device_id=partner,
            device_id_type=mesh_ids,
        )
        for n, dst in enumerate((wg, wu, wdn))
    ]
    for copy in small:
        copy.start()
    load_start(0)
    load_start(1)
    for copy in small:
        copy.wait()
    load_start(2)

    normed = rms_scale(tokens[...].astype(F32), attn_gain[...]).astype(BF16)

    def rounded(weight):
        return jnp.dot(normed, weight, preferred_element_type=F32).astype(BF16).astype(F32)

    xa = nt_dot(normed, wd[...]).astype(BF16).astype(F32) + bias[...]
    fade = jnp.exp(-rate[...] * (jnp.maximum(xa, 0.0) + jnp.log1p(jnp.exp(-jnp.abs(xa)))))
    beta = jax.nn.sigmoid(nt_dot(normed, wb[...]).astype(BF16).astype(F32))
    for h in range(heads):
        fades[:, h, :] = jnp.broadcast_to(fade[:, h : h + 1], (seqs, dim))
        betas[:, h, :] = jnp.broadcast_to(beta[:, h : h + 1], (seqs, dim))

    eye = iota((seqs, seqs), 1) == iota((seqs, seqs), 0)

    def column(row):
        return jnp.sum(jnp.where(eye, row, 0.0), axis=1, keepdims=True)

    lower = (iota((seqs, seqs), 1) < iota((seqs, seqs), 0)).astype(BF16)
    slots = n_ep * cap
    taken = jnp.zeros((1, n_ep), F32)
    found = []
    mine = jnp.zeros((seqs, slots), F32)
    for j in range(top):
        route = column(routes[j : j + 1, :].astype(F32)).astype(jnp.int32)
        hot = (iota((seqs, n_ep), 1) == route).astype(F32)
        before = jnp.dot(lower, hot.astype(BF16), preferred_element_type=F32) + taken
        slot = jnp.sum(before * hot, axis=1, keepdims=True).astype(jnp.int32)
        taken = taken + jnp.sum(hot, axis=0, keepdims=True)
        place = route * cap + slot + jnp.where(slot < shares[0], 0, slots - shares[0])
        found.append((iota((seqs, n_tp * slots), 1) == place).astype(F32))
        mine = mine + (iota((seqs, slots), 1) + t * slots == place).astype(F32)
    spread[...] = mine.T.astype(BF16)
    picks[...] = jnp.concatenate(found, axis=0).astype(BF16)

    load_wait(0)
    for c in range(chunks // 3):
        in_copy(c).start()
    raw_q = rounded(wbuf[0])
    load_wait(1)
    for c in range(chunks // 3, 2 * chunks // 3):
        in_copy(c).start()
    raw_k = rounded(wbuf[1])
    for h in range(heads):
        span = slice(h * dim, (h + 1) * dim)
        query = unit_rows(silu(raw_q[:, span])) * dim ** (-0.5)
        key = unit_rows(silu(raw_k[:, span]))
        kq[:, h, :] = key
        turned[h] = key.T
        kq[:, heads + h, :] = query
        dots[:, h, :] = jnp.broadcast_to(jnp.sum(key * query, axis=-1, keepdims=True), (seqs, dim))
    load_wait(2)
    for c in range(2 * chunks // 3, chunks):
        in_copy(c).start()
    value = silu(rounded(wbuf[2]))
    for h in range(heads):
        vals[:, h, :] = value[:, h * dim : (h + 1) * dim]

    def hits_of(c):
        in_copy(c).wait()
        hits = []
        for s in range(c * step, (c + 1) * step):
            lhs = kq[s].astype(BF16)
            hits.append([jnp.dot(lhs, ns[s, h].astype(BF16), preferred_element_type=F32) for h in range(heads)])
        return hits

    def update(c, hits):
        for i in range(step):
            s = c * step + i
            fs, bs, vs, ds = fades[s], betas[s], vals[s], dots[s]
            for h in range(heads):
                hit = hits[i][h]
                f = fs[h : h + 1]
                written = bs[h : h + 1] * (vs[h : h + 1] - f * hit[h : h + 1])
                kc = jnp.broadcast_to(turned[h, :, s : s + 1], (dim, dim))
                ns[s, h] = f * ns[s, h] + kc * written
                reads[s, pl.ds(h, 1)] = f * hit[heads + h : heads + h + 1] + written * ds[h : h + 1]

    before = None
    for c in range(chunks):
        hits = hits_of(c)
        if c == 0:
            load_start(3)
        if c == min(2, chunks - 1):
            load_start(4)
        if before is not None:
            update(c - 1, before)
        before = hits
    update(chunks - 1, before)
    for copy in experts:
        copy.start()
    load_wait(3)
    zbuf[...] = silu(rounded(wbuf[3]))
    mixed = []
    for h in range(heads):
        span = slice(h * dim, (h + 1) * dim)
        mixed.append((rms_scale(reads[:, h, :], out_gain[...]) * zbuf[:, span]).astype(BF16))
    load_wait(4)
    part_out[...] = jnp.dot(jnp.concatenate(mixed, axis=1), wo[...], preferred_element_type=F32).astype(BF16)
    pl.semaphore_wait(barrier, n_ep)

    swap = pltpu.make_async_remote_copy(
        src_ref=part_out,
        dst_ref=part_in,
        send_sem=part_sem.at[0],
        recv_sem=part_sem.at[1],
        device_id=partner,
        device_id_type=mesh_ids,
    )
    swap.start()
    experts[0].wait()
    push[0].start()
    swap.wait()
    rows = tokens[...].astype(F32) + (part_out[...].astype(F32) + part_in[...].astype(F32))
    resid[...] = rows
    moe = rms_scale(rows, ffn_gain[...]).astype(BF16)
    going = jnp.dot(spread[...], moe, preferred_element_type=F32)
    disp[...] = going.reshape(n_ep, cap, width).astype(BF16)

    def go(n, p):
        return pltpu.make_async_remote_copy(
            src_ref=disp.at[p, pl.ds(0, n)],
            dst_ref=arrived.at[e, pl.ds(0, n)],
            send_sem=go_sem.at[0],
            recv_sem=go_sem.at[1],
            device_id={"ep": p, "tp": t},
            device_id_type=mesh_ids,
        )

    def all_go(n, which):
        block = arrived.at[pl.ds(0, n_ep - 1), pl.ds(0, n)]
        return pltpu.make_async_copy(block, block, go_sem.at[which])

    def back(n, c, p):
        return pltpu.make_async_remote_copy(
            src_ref=ret_out.at[c, p, pl.ds(0, n)],
            dst_ref=ret_in.at[t, e, pl.ds(0, n)],
            send_sem=back_sem.at[0],
            recv_sem=back_recv.at[t],
            device_id={"ep": p, "tp": c},
            device_id_type=mesh_ids,
        )

    def all_back(n, c, count, sem):
        block = ret_in.at[c, pl.ds(0, count), pl.ds(0, n)]
        return pltpu.make_async_copy(block, block, sem)

    for c, n in enumerate(shares):
        if n:

            @pl.when(t == c)
            def _(n=n):
                lax.fori_loop(0, n_ep - 1, lambda i, carry: (go(n, across(i)).start(), carry)[1], 0)

    arrived[e] = disp[e]
    for n in (1, 2):
        experts[n].wait()
        push[n].start()
    for c, n in enumerate(shares):
        if n:

            @pl.when(t == c)
            def _(n=n):
                all_go(n, 1).wait()

    got = arrived[...].astype(F32).reshape(slots, width).astype(BF16)
    push[0].wait_recv()
    gates = [jnp.dot(got, wg[h], preferred_element_type=F32) for h in range(n_tp)]
    push[1].wait_recv()
    ups = [jnp.dot(got, wu[h], preferred_element_type=F32) for h in range(n_tp)]
    hidden = [(silu(gates[h]) * ups[h]).astype(BF16) for h in range(n_tp)]
    push[2].wait_recv()
    for c in range(n_tp):
        term = None
        for h in range(n_tp):
            piece = jnp.dot(hidden[h], wdn[h, :, c * cols : (c + 1) * cols], preferred_element_type=F32)
            term = piece if term is None else term + piece
        ret_out[c] = term.reshape(n_ep, cap, cols).astype(BF16)

    for c, n in enumerate(shares):
        if n:

            @pl.when(t == c)
            def _(n=n, c=c):
                def send(i, carry):
                    for d in range(n_tp):
                        back(n, d, rising(i)).start()
                    return carry

                lax.fori_loop(0, n_ep - 1, send, 0)
                for d in range(n_tp):
                    if d != c:
                        back(n, d, e).start()

    ret_in[t, e] = ret_out[t, e]
    total = resid[:, pl.ds(pl.multiple_of(t * cols, 128), cols)]
    scale = [column(weights[j : j + 1, :]) for j in range(top)]
    for c, n in enumerate(shares):
        if n:
            for d in range(n_tp):

                @pl.when(t == d)
                def _(n=n, c=c, d=d):
                    all_back(n, c, n_ep - (c == d), back_recv.at[c]).wait()

    kept = [(iota((n_ep, cap, cols), 1) < n) for n in shares]
    returned = [
        jnp.where(kept[c], ret_in[c].astype(F32), 0.0).reshape(slots, cols).astype(BF16) for c in range(n_tp)
    ]
    combined = jnp.dot(picks[...], jnp.concatenate(returned, axis=0), preferred_element_type=F32)
    for j in range(top):
        total = total + combined[j * seqs : (j + 1) * seqs] * scale[j]
    out[...] = total.astype(BF16)

    for copy in push:
        copy.wait_send()
    for c, n in enumerate(shares):
        if n:

            @pl.when(t == c)
            def _(n=n):
                all_go(n, 0).wait()
                for d in range(n_tp):
                    all_back(n, d, n_ep - 1 + d, back_sem.at[0]).wait()


def flush_kernel(step, out_ref, ns_ref, out, ns, sem):
    copies = [pltpu.make_async_copy(out_ref, out, sem.at[0])]
    for s in range(0, ns.shape[0], step):
        rows = pl.ds(s, step)
        copies.append(pltpu.make_async_copy(ns_ref.at[rows], ns.at[rows], sem.at[1]))
    for copy in copies:
        copy.start()
    copies[0].wait()
    pltpu.make_async_copy(ns_ref, ns, sem.at[1]).wait()


def per_device(
    n_ep,
    n_tp,
    tokens,
    attn_gain,
    w_query,
    w_key,
    w_value,
    w_zgate,
    w_decay,
    w_beta,
    decay_rate,
    decay_bias,
    state,
    out_gain,
    w_out,
    ffn_gain,
    expert_gate,
    expert_up,
    expert_down,
    routes,
    route_weight,
):
    seqs, width = tokens.shape
    heads, dim = state.shape[1], state.shape[2]
    top = routes.shape[1]
    inner = heads * dim
    step = 4 if seqs % 4 == 0 else 1
    chunks = seqs // step
    live = max(2, 2 * seqs * top // n_ep)
    first = 2 * -(-live // 4)
    shares = (first, live - first)
    cap = -(-first // 8) * 8
    cols = width // n_tp
    ff = expert_gate.shape[2]
    slots = n_ep * cap
    vmem = pltpu.VMEM
    dma = pltpu.SemaphoreType.DMA
    layer_out, new_state = pl.pallas_call(
        functools.partial(layer_kernel, n_ep, n_tp, top, cap, shares, step),
        out_shape=(vmem((seqs, cols), BF16), vmem(state.shape, F32)),
        in_specs=[HBM] * 19,
        out_specs=(VMEM, VMEM),
        scratch_shapes=[
            vmem((seqs, width), BF16),
            vmem((1, width), F32),
            vmem((heads, width), BF16),
            vmem((heads, width), BF16),
            vmem((1, heads), F32),
            vmem((1, heads), F32),
            vmem((1, dim), F32),
            vmem((1, width), F32),
            vmem((top, seqs), jnp.int32),
            vmem((top, seqs), F32),
            vmem((4, width, inner), BF16),
            vmem((inner, width), BF16),
            vmem((n_tp, width, ff), BF16),
            vmem((n_tp, width, ff), BF16),
            vmem((n_tp, ff, width), BF16),
            vmem((seqs, 2 * heads, dim), F32),
            vmem((seqs, heads, dim), F32),
            vmem((seqs, inner), F32),
            vmem((seqs, heads, dim), F32),
            vmem((seqs, heads, dim), F32),
            vmem((seqs, heads, dim), F32),
            vmem((heads, dim, seqs), F32),
            vmem((seqs, heads, dim), F32),
            vmem((slots, seqs), BF16),
            vmem((top * seqs, n_tp * slots), BF16),
            vmem((seqs, width), BF16),
            vmem((seqs, width), BF16),
            vmem((seqs, width), F32),
            vmem((n_ep, cap, width), BF16),
            vmem((n_ep, cap, width), BF16),
            vmem((n_tp, n_ep, cap, cols), BF16),
            vmem((n_tp, n_ep, cap, cols), BF16),
            dma((10,)),
            dma((5,)),
            dma((chunks,)),
            dma((3,)),
            dma((2,)),
            dma((2, 3)),
            dma((2,)),
            dma((1,)),
            dma((n_tp,)),
        ],
        compiler_params=pltpu.CompilerParams(
            collective_id=0, has_side_effects=True, vmem_limit_bytes=VMEM_LIMIT
        ),
        name="layer",
    )(
        tokens,
        attn_gain.reshape(1, width),
        w_decay.T,
        w_beta.T,
        decay_rate.reshape(1, heads),
        decay_bias.reshape(1, heads),
        out_gain.reshape(1, dim),
        ffn_gain.reshape(1, width),
        routes.T,
        route_weight.T,
        w_query,
        w_key,
        w_value,
        w_zgate,
        state,
        w_out,
        expert_gate,
        expert_up,
        expert_down,
    )
    return pl.pallas_call(
        functools.partial(flush_kernel, step),
        out_shape=(jax.ShapeDtypeStruct((seqs, cols), BF16), jax.ShapeDtypeStruct(state.shape, F32)),
        in_specs=[VMEM, VMEM],
        out_specs=(HBM, HBM),
        scratch_shapes=[dma((2,))],
        compiler_params=pltpu.CompilerParams(vmem_limit_bytes=2**20),
        name="flush",
    )(
        pltpu.with_memory_space_constraint(layer_out, pltpu.VMEM),
        pltpu.with_memory_space_constraint(new_state, pltpu.VMEM),
    )


def solution(mesh):
    in_specs = (
        P("ep", None),
        P(),
        P(None, "tp"),
        P(None, "tp"),
        P(None, "tp"),
        P(None, "tp"),
        P(None, "tp"),
        P(None, "tp"),
        P("tp"),
        P("tp"),
        P("ep", "tp", None, None),
        P(),
        P("tp", None),
        P(),
        P("ep", None, "tp"),
        P("ep", None, "tp"),
        P("ep", "tp", None),
        P("ep", None),
        P("ep", None),
    )
    out_specs = (P("ep", "tp"), P("ep", "tp", None, None))
    body = functools.partial(per_device, mesh.shape["ep"], mesh.shape["tp"])
    return jax.shard_map(body, mesh=mesh, in_specs=in_specs, out_specs=out_specs, check_vma=False)
```

```python
import functools

import jax
import jax.numpy as jnp
from jax import lax
from jax.experimental import pallas as pl
from jax.experimental.pallas import tpu as pltpu
from jax.sharding import PartitionSpec as P

EPS = 1e-06
F32 = jnp.float32
BF16 = jnp.bfloat16
CUTS = (6,)
VMEM_LIMIT = 57 * 1024 * 1024
HBM = pl.BlockSpec(memory_space=pltpu.HBM)
VMEM = pl.BlockSpec(memory_space=pltpu.VMEM)


def rms_scale(rows, gain):
    return rows * lax.rsqrt(jnp.mean(rows * rows, axis=-1, keepdims=True) + EPS) * gain


def unit_rows(rows):
    return rows * lax.rsqrt(jnp.sum(rows * rows, axis=-1, keepdims=True) + EPS)


def silu(x):
    return x * jax.nn.sigmoid(x)


def nt_dot(rows, weight):
    return lax.dot_general(rows, weight, (((1,), (1,)), ((), ())), preferred_element_type=F32)


def iota(shape, axis):
    return lax.broadcasted_iota(jnp.int32, shape, axis)


def layer_kernel(
    n_ep,
    n_tp,
    top,
    cap,
    shares,
    step,
    order,
    bounds,
    tokens_ref,
    attn_ref,
    wd_ref,
    wb_ref,
    rate_ref,
    bias_ref,
    og_ref,
    ffn_ref,
    routes_ref,
    weights_ref,
    wq,
    wk,
    wv,
    wz,
    state,
    w_out,
    w_gate,
    w_up,
    w_down,
    out,
    ns,
    tokens,
    attn_gain,
    wd,
    wb,
    rate,
    bias,
    out_gain,
    ffn_gain,
    routes,
    weights,
    wbuf,
    wo,
    wg,
    wu,
    wdn,
    kq,
    vals,
    zbuf,
    fades,
    betas,
    dots,
    turned,
    reads,
    spread,
    picks,
    part_out,
    part_in,
    resid,
    disp,
    arrived,
    ret_out,
    ret_in,
    small_sem,
    w_sem,
    in_sem,
    x_sem,
    part_sem,
    push_sem,
    go_sem,
    back_sem,
    back_recv,
):
    seqs, heads, dim, _ = ns.shape
    width = tokens.shape[1]
    cols = width // n_tp
    chunks = seqs // step
    e = lax.axis_index("ep")
    t = lax.axis_index("tp")
    u = n_tp - 1 - t
    mesh_ids = pl.DeviceIdType.MESH
    partner = {"ep": e, "tp": u}
    barrier = pltpu.get_barrier_semaphore()
    pl.semaphore_signal(barrier, inc=1, device_id=partner, device_id_type=mesh_ids)

    groups = len(bounds) - 1
    rank = sum((jnp.where(e == p, k, 0) for k, p in enumerate(order)), 0)
    mine_group = sum((jnp.where(rank >= b, 1, 0) for b in bounds[1:-1]), 0)
    bits = [1 << k for k in range((n_ep - 1).bit_length())] if n_ep & (n_ep - 1) == 0 else []
    flips = [(b, b * (1 - 2 * lax.rem(e // b, 2))) for b in bits]

    def peer(i):
        return sum((flip for b, flip in flips if (n_ep - i) & b), e) if bits else lax.rem(e + i, n_ep)

    def greet(i, carry):
        p = lax.rem(e + 1 + i, n_ep)
        pl.semaphore_signal(barrier, inc=1, device_id={"ep": p, "tp": t}, device_id_type=mesh_ids)
        return carry

    lax.fori_loop(0, n_ep - 1, greet, 0)

    def in_copy(c):
        rows = pl.ds(c * step, step)
        return pltpu.make_async_copy(state.at[rows], ns.at[rows], in_sem.at[c])

    small = [
        pltpu.make_async_copy(src, dst, small_sem.at[n])
        for n, (src, dst) in enumerate(
            (
                (tokens_ref, tokens),
                (attn_ref, attn_gain),
                (wd_ref, wd),
                (wb_ref, wb),
                (rate_ref, rate),
                (bias_ref, bias),
                (og_ref, out_gain),
                (ffn_ref, ffn_gain),
                (routes_ref, routes),
                (weights_ref, weights),
            )
        )
    ]
    weight = [(src, wbuf.at[n]) for n, src in enumerate((wq, wk, wv, wz))] + [(w_out, wo)]

    def load_start(n):
        pltpu.make_async_copy(*weight[n], w_sem.at[n]).start()

    def load_wait(n):
        pltpu.make_async_copy(*weight[n], w_sem.at[n]).wait()

    experts = [
        pltpu.make_async_copy(src.at[0], dst.at[t], x_sem.at[n])
        for n, (src, dst) in enumerate(((w_gate, wg), (w_up, wu), (w_down, wdn)))
    ]
    push = [
        pltpu.make_async_remote_copy(
            src_ref=dst.at[t],
            dst_ref=dst.at[t],
            send_sem=push_sem.at[0, n],
            recv_sem=push_sem.at[1, n],
            device_id=partner,
            device_id_type=mesh_ids,
        )
        for n, dst in enumerate((wg, wu, wdn))
    ]
    for copy in small:
        copy.start()
    load_start(0)
    load_start(1)
    for copy in small:
        copy.wait()
    load_start(2)

    normed = rms_scale(tokens[...].astype(F32), attn_gain[...]).astype(BF16)

    def rounded(weight):
        return jnp.dot(normed, weight, preferred_element_type=F32).astype(BF16).astype(F32)

    xa = nt_dot(normed, wd[...]).astype(BF16).astype(F32) + bias[...]
    fade = jnp.exp(-rate[...] * (jnp.maximum(xa, 0.0) + jnp.log1p(jnp.exp(-jnp.abs(xa)))))
    beta = jax.nn.sigmoid(nt_dot(normed, wb[...]).astype(BF16).astype(F32))
    for h in range(heads):
        fades[:, h, :] = jnp.broadcast_to(fade[:, h : h + 1], (seqs, dim))
        betas[:, h, :] = jnp.broadcast_to(beta[:, h : h + 1], (seqs, dim))

    eye = iota((seqs, seqs), 1) == iota((seqs, seqs), 0)

    def column(row):
        return jnp.sum(jnp.where(eye, row, 0.0), axis=1, keepdims=True)

    lower = (iota((seqs, seqs), 1) < iota((seqs, seqs), 0)).astype(BF16)
    slots = n_ep * cap
    taken = jnp.zeros((1, n_ep), F32)
    found = []
    mine = jnp.zeros((seqs, slots), F32)
    for j in range(top):
        route = column(routes[j : j + 1, :].astype(F32)).astype(jnp.int32)
        hot = (iota((seqs, n_ep), 1) == route).astype(F32)
        before = jnp.dot(lower, hot.astype(BF16), preferred_element_type=F32) + taken
        slot = jnp.sum(before * hot, axis=1, keepdims=True).astype(jnp.int32)
        taken = taken + jnp.sum(hot, axis=0, keepdims=True)
        place = route * cap + slot + jnp.where(slot < shares[0], 0, slots - shares[0])
        found.append((iota((seqs, n_tp * slots), 1) == place).astype(F32))
        mine = mine + (iota((seqs, slots), 1) + t * slots == place).astype(F32)
    spread[...] = mine.T.astype(BF16)
    picks[...] = jnp.concatenate(found, axis=0).astype(BF16)

    load_wait(0)
    for c in range(chunks // 3):
        in_copy(c).start()
    raw_q = rounded(wbuf[0])
    load_wait(1)
    for c in range(chunks // 3, 2 * chunks // 3):
        in_copy(c).start()
    raw_k = rounded(wbuf[1])
    for h in range(heads):
        span = slice(h * dim, (h + 1) * dim)
        query = unit_rows(silu(raw_q[:, span])) * dim ** (-0.5)
        key = unit_rows(silu(raw_k[:, span]))
        kq[:, h, :] = key
        turned[h] = key.T
        kq[:, heads + h, :] = query
        dots[:, h, :] = jnp.broadcast_to(jnp.sum(key * query, axis=-1, keepdims=True), (seqs, dim))
    load_wait(2)
    load_start(3)
    for c in range(2 * chunks // 3, chunks):
        in_copy(c).start()
    value = silu(rounded(wbuf[2]))
    for h in range(heads):
        vals[:, h, :] = value[:, h * dim : (h + 1) * dim]

    def hits_of(c):
        in_copy(c).wait()
        hits = []
        for s in range(c * step, (c + 1) * step):
            lhs = kq[s].astype(BF16)
            hits.append([jnp.dot(lhs, ns[s, h].astype(BF16), preferred_element_type=F32) for h in range(heads)])
        return hits

    def update(c, hits):
        for i in range(step):
            s = c * step + i
            fs, bs, vs, ds = fades[s], betas[s], vals[s], dots[s]
            for h in range(heads):
                hit = hits[i][h]
                f = fs[h : h + 1]
                written = bs[h : h + 1] * (vs[h : h + 1] - f * hit[h : h + 1])
                kc = jnp.broadcast_to(turned[h, :, s : s + 1], (dim, dim))
                ns[s, h] = f * ns[s, h] + kc * written
                reads[s, pl.ds(h, 1)] = f * hit[heads + h : heads + h + 1] + written * ds[h : h + 1]

    before = None
    zc = max(chunks - 2, 0)
    for c in range(chunks):
        hits = hits_of(c)
        if c == min(1, chunks - 1):
            load_start(4)
        if c == chunks - 1:
            experts[0].start()
        if c == zc:
            load_wait(3)
            zbuf[...] = silu(rounded(wbuf[3]))
        if before is not None:
            update(c - 1, before)
        before = hits
    update(chunks - 1, before)
    for copy in experts[1:]:
        copy.start()
    mixed = []
    for h in range(heads):
        span = slice(h * dim, (h + 1) * dim)
        mixed.append((rms_scale(reads[:, h, :], out_gain[...]) * zbuf[:, span]).astype(BF16))
    load_wait(4)
    part_out[...] = jnp.dot(jnp.concatenate(mixed, axis=1), wo[...], preferred_element_type=F32).astype(BF16)
    pl.semaphore_wait(barrier, n_ep)

    swap = pltpu.make_async_remote_copy(
        src_ref=part_out,
        dst_ref=part_in,
        send_sem=part_sem.at[0],
        recv_sem=part_sem.at[1],
        device_id=partner,
        device_id_type=mesh_ids,
    )
    swap.start()
    experts[0].wait()
    push[0].start()
    swap.wait_recv()
    rows = tokens[...].astype(F32) + (part_out[...].astype(F32) + part_in[...].astype(F32))
    resid[...] = rows
    moe = rms_scale(rows, ffn_gain[...]).astype(BF16)
    going = jnp.dot(spread[...], moe, preferred_element_type=F32)
    disp[...] = going.reshape(n_ep, cap, width).astype(BF16)

    def go(n, p):
        return pltpu.make_async_remote_copy(
            src_ref=disp.at[p, pl.ds(0, n)],
            dst_ref=arrived.at[rank, pl.ds(0, n)],
            send_sem=go_sem.at[groups],
            recv_sem=go_sem.at[mine_group],
            device_id={"ep": p, "tp": t},
            device_id_type=mesh_ids,
        )

    def all_go(n, count, which):
        block = arrived.at[pl.ds(0, count), pl.ds(0, n)]
        return pltpu.make_async_copy(block, block, go_sem.at[which])

    def back(n, c, k):
        return pltpu.make_async_remote_copy(
            src_ref=ret_out.at[c, k, pl.ds(0, n)],
            dst_ref=ret_in.at[t, e, pl.ds(0, n)],
            send_sem=back_sem.at[0],
            recv_sem=back_recv.at[t],
            device_id={"ep": order[k], "tp": c},
            device_id_type=mesh_ids,
        )

    def all_back(n, c, count, sem):
        block = ret_in.at[c, pl.ds(0, count), pl.ds(0, n)]
        return pltpu.make_async_copy(block, block, sem)

    for c, n in enumerate(shares):
        if n:

            @pl.when(t == c)
            def _(n=n):
                for i in range(1, n_ep):
                    go(n, peer(i)).start()

    arrived[rank] = disp[e]
    for n in (1, 2):
        experts[n].wait()
        push[n].start()
    for g in range(groups):
        low, high = bounds[g], bounds[g + 1]
        size = high - low
        span = pl.ds(low, size)
        for c, n in enumerate(shares):
            if n:

                @pl.when((t == c) & (mine_group == g))
                def _(n=n, g=g, size=size):
                    if size > 1:
                        all_go(n, size - 1, g).wait()

                @pl.when((t == c) & (mine_group != g))
                def _(n=n, g=g, size=size):
                    all_go(n, size, g).wait()

        got = arrived[span].astype(F32).reshape(size * cap, width).astype(BF16)
        if g == 0:
            push[0].wait_recv()
        gates = [jnp.dot(got, wg[h], preferred_element_type=F32) for h in range(n_tp)]
        if g == 0:
            push[1].wait_recv()
        ups = [jnp.dot(got, wu[h], preferred_element_type=F32) for h in range(n_tp)]
        hidden = [(silu(gates[h]) * ups[h]).astype(BF16) for h in range(n_tp)]
        if g == 0:
            push[2].wait_recv()
        for d in range(n_tp):
            term = None
            for h in range(n_tp):
                piece = jnp.dot(hidden[h], wdn[h, :, d * cols : (d + 1) * cols], preferred_element_type=F32)
                term = piece if term is None else term + piece
            ret_out[d, span] = term.reshape(size, cap, cols).astype(BF16)
            for c, n in enumerate(shares):
                if n:

                    @pl.when(t == c)
                    def _(n=n, c=c, d=d, low=low, high=high):
                        for k in range(low, high):
                            if d != c:
                                back(n, d, k).start()
                            else:

                                @pl.when(e != order[k])
                                def _(k=k):
                                    back(n, d, k).start()

    ret_in[t, e] = ret_out[t, rank]
    total = resid[:, pl.ds(pl.multiple_of(t * cols, 128), cols)]
    scale = [column(weights[j : j + 1, :]) for j in range(top)]
    for c, n in enumerate(shares):
        if n:
            for d in range(n_tp):

                @pl.when(t == d)
                def _(n=n, c=c, d=d):
                    all_back(n, c, n_ep - (c == d), back_recv.at[c]).wait()

    kept = [(iota((n_ep, cap, cols), 1) < n) for n in shares]
    returned = [
        jnp.where(kept[c], ret_in[c].astype(F32), 0.0).reshape(slots, cols).astype(BF16) for c in range(n_tp)
    ]
    combined = jnp.dot(picks[...], jnp.concatenate(returned, axis=0), preferred_element_type=F32)
    for j in range(top):
        total = total + combined[j * seqs : (j + 1) * seqs] * scale[j]
    out[...] = total.astype(BF16)

    for copy in (swap, *push):
        copy.wait_send()
    for c, n in enumerate(shares):
        if n:

            @pl.when(t == c)
            def _(n=n):
                all_go(n, n_ep - 1, groups).wait()
                for d in range(n_tp):
                    all_back(n, d, n_ep - 1 + d, back_sem.at[0]).wait()


def flush_kernel(step, out_ref, ns_ref, out, ns, sem):
    copies = [pltpu.make_async_copy(out_ref, out, sem.at[0])]
    for s in range(0, ns.shape[0], step):
        rows = pl.ds(s, step)
        copies.append(pltpu.make_async_copy(ns_ref.at[rows], ns.at[rows], sem.at[1]))
    for copy in copies:
        copy.start()
    copies[0].wait()
    pltpu.make_async_copy(ns_ref, ns, sem.at[1]).wait()


def per_device(
    n_ep,
    n_tp,
    order,
    tokens,
    attn_gain,
    w_query,
    w_key,
    w_value,
    w_zgate,
    w_decay,
    w_beta,
    decay_rate,
    decay_bias,
    state,
    out_gain,
    w_out,
    ffn_gain,
    expert_gate,
    expert_up,
    expert_down,
    routes,
    route_weight,
):
    seqs, width = tokens.shape
    heads, dim = state.shape[1], state.shape[2]
    top = routes.shape[1]
    inner = heads * dim
    step = 4 if seqs % 4 == 0 else 1
    chunks = seqs // step
    live = max(2, 2 * seqs * top // n_ep)
    most = 2 * -(-live // 4)
    shares = (live - most, most)
    cap = -(-most // 8) * 8
    bounds = sorted({0, n_ep, *(n_ep * share // 16 for share in CUTS)})
    groups = len(bounds) - 1
    cols = width // n_tp
    ff = expert_gate.shape[2]
    slots = n_ep * cap
    vmem = pltpu.VMEM
    dma = pltpu.SemaphoreType.DMA
    layer_out, new_state = pl.pallas_call(
        functools.partial(layer_kernel, n_ep, n_tp, top, cap, shares, step, order, bounds),
        out_shape=(vmem((seqs, cols), BF16), vmem(state.shape, F32)),
        in_specs=[HBM] * 19,
        out_specs=(VMEM, VMEM),
        scratch_shapes=[
            vmem((seqs, width), BF16),
            vmem((1, width), F32),
            vmem((heads, width), BF16),
            vmem((heads, width), BF16),
            vmem((1, heads), F32),
            vmem((1, heads), F32),
            vmem((1, dim), F32),
            vmem((1, width), F32),
            vmem((top, seqs), jnp.int32),
            vmem((top, seqs), F32),
            vmem((4, width, inner), BF16),
            vmem((inner, width), BF16),
            vmem((n_tp, width, ff), BF16),
            vmem((n_tp, width, ff), BF16),
            vmem((n_tp, ff, width), BF16),
            vmem((seqs, 2 * heads, dim), F32),
            vmem((seqs, heads, dim), F32),
            vmem((seqs, inner), F32),
            vmem((seqs, heads, dim), F32),
            vmem((seqs, heads, dim), F32),
            vmem((seqs, heads, dim), F32),
            vmem((heads, dim, seqs), F32),
            vmem((seqs, heads, dim), F32),
            vmem((slots, seqs), BF16),
            vmem((top * seqs, n_tp * slots), BF16),
            vmem((seqs, width), BF16),
            vmem((seqs, width), BF16),
            vmem((seqs, width), F32),
            vmem((n_ep, cap, width), BF16),
            vmem((n_ep, cap, width), BF16),
            vmem((n_tp, n_ep, cap, cols), BF16),
            vmem((n_tp, n_ep, cap, cols), BF16),
            dma((10,)),
            dma((5,)),
            dma((chunks,)),
            dma((3,)),
            dma((2,)),
            dma((2, 3)),
            dma((groups + 1,)),
            dma((1,)),
            dma((n_tp,)),
        ],
        compiler_params=pltpu.CompilerParams(
            collective_id=0, has_side_effects=True, vmem_limit_bytes=VMEM_LIMIT
        ),
        name="layer",
    )(
        tokens,
        attn_gain.reshape(1, width),
        w_decay.T,
        w_beta.T,
        decay_rate.reshape(1, heads),
        decay_bias.reshape(1, heads),
        out_gain.reshape(1, dim),
        ffn_gain.reshape(1, width),
        routes.T,
        route_weight.T,
        w_query,
        w_key,
        w_value,
        w_zgate,
        state,
        w_out,
        expert_gate,
        expert_up,
        expert_down,
    )
    return pl.pallas_call(
        functools.partial(flush_kernel, step),
        out_shape=(jax.ShapeDtypeStruct((seqs, cols), BF16), jax.ShapeDtypeStruct(state.shape, F32)),
        in_specs=[VMEM, VMEM],
        out_specs=(HBM, HBM),
        scratch_shapes=[dma((2,))],
        compiler_params=pltpu.CompilerParams(vmem_limit_bytes=2**20),
        name="flush",
    )(
        pltpu.with_memory_space_constraint(layer_out, pltpu.VMEM),
        pltpu.with_memory_space_constraint(new_state, pltpu.VMEM),
    )


def solution(mesh):
    in_specs = (
        P("ep", None),
        P(),
        P(None, "tp"),
        P(None, "tp"),
        P(None, "tp"),
        P(None, "tp"),
        P(None, "tp"),
        P(None, "tp"),
        P("tp"),
        P("tp"),
        P("ep", "tp", None, None),
        P(),
        P("tp", None),
        P(),
        P("ep", None, "tp"),
        P("ep", None, "tp"),
        P("ep", "tp", None),
        P("ep", None),
        P("ep", None),
    )
    out_specs = (P("ep", "tp"), P("ep", "tp", None, None))
    n_ep, n_tp = mesh.shape["ep"], mesh.shape["tp"]
    chips = mesh.devices.reshape(n_ep, n_tp)[:, 0]
    order = sorted(range(n_ep), key=lambda p: sum(getattr(chips[p], "coords", (p,))))
    body = functools.partial(per_device, n_ep, n_tp, order)
    return jax.shard_map(body, mesh=mesh, in_specs=in_specs, out_specs=out_specs, check_vma=False)
```

```python
import functools

import jax
import jax.numpy as jnp
from jax import lax
from jax.experimental import pallas as pl
from jax.experimental.pallas import tpu as pltpu
from jax.sharding import PartitionSpec as P

EPS = 1e-06
F32 = jnp.float32
BF16 = jnp.bfloat16
CUTS = (4,)
VMEM_LIMIT = 57 * 1024 * 1024
HBM = pl.BlockSpec(memory_space=pltpu.HBM)
VMEM = pl.BlockSpec(memory_space=pltpu.VMEM)


def rms_scale(rows, gain):
    return rows * lax.rsqrt(jnp.mean(rows * rows, axis=-1, keepdims=True) + EPS) * gain


def unit_rows(rows):
    return rows * lax.rsqrt(jnp.sum(rows * rows, axis=-1, keepdims=True) + EPS)


def silu(x):
    return x * jax.nn.sigmoid(x)


def nt_dot(rows, weight):
    return lax.dot_general(rows, weight, (((1,), (1,)), ((), ())), preferred_element_type=F32)


def iota(shape, axis):
    return lax.broadcasted_iota(jnp.int32, shape, axis)


def layer_kernel(
    n_ep,
    n_tp,
    top,
    cap,
    shares,
    step,
    order,
    bounds,
    tokens_ref,
    attn_ref,
    wd_ref,
    wb_ref,
    rate_ref,
    bias_ref,
    og_ref,
    ffn_ref,
    routes_ref,
    weights_ref,
    wq,
    wk,
    wv,
    wz,
    state,
    w_out,
    w_gate,
    w_up,
    w_down,
    out,
    ns,
    tokens,
    attn_gain,
    wd,
    wb,
    rate,
    bias,
    out_gain,
    ffn_gain,
    routes,
    weights,
    wbuf,
    wo,
    wg,
    wu,
    wdn,
    kq,
    vals,
    zbuf,
    fades,
    betas,
    dots,
    turned,
    reads,
    spread,
    picks,
    part_out,
    part_in,
    resid,
    disp,
    arrived,
    ret_out,
    ret_in,
    small_sem,
    w_sem,
    in_sem,
    x_sem,
    part_sem,
    push_sem,
    go_sem,
    back_sem,
    back_recv,
):
    seqs, heads, dim, _ = ns.shape
    width = tokens.shape[1]
    cols = width // n_tp
    chunks = seqs // step
    e = lax.axis_index("ep")
    t = lax.axis_index("tp")
    u = n_tp - 1 - t
    mesh_ids = pl.DeviceIdType.MESH
    partner = {"ep": e, "tp": u}
    barrier = pltpu.get_barrier_semaphore()
    pl.semaphore_signal(barrier, inc=1, device_id=partner, device_id_type=mesh_ids)

    groups = len(bounds) - 1
    rank = sum((jnp.where(e == p, k, 0) for k, p in enumerate(order)), 0)
    mine_group = sum((jnp.where(rank >= b, 1, 0) for b in bounds[1:-1]), 0)
    bits = [1 << k for k in range((n_ep - 1).bit_length())] if n_ep & (n_ep - 1) == 0 else []
    flips = [(b, b * (1 - 2 * lax.rem(e // b, 2))) for b in bits]

    def peer(i):
        return sum((flip for b, flip in flips if (n_ep - i) & b), e) if bits else lax.rem(e + i, n_ep)

    def greet(i, carry):
        p = lax.rem(e + 1 + i, n_ep)
        pl.semaphore_signal(barrier, inc=1, device_id={"ep": p, "tp": t}, device_id_type=mesh_ids)
        return carry

    lax.fori_loop(0, n_ep - 1, greet, 0)

    def in_copy(c):
        rows = pl.ds(c * step, step)
        return pltpu.make_async_copy(state.at[rows], ns.at[rows], in_sem.at[c])

    small = [
        pltpu.make_async_copy(src, dst, small_sem.at[n])
        for n, (src, dst) in enumerate(
            (
                (tokens_ref, tokens),
                (attn_ref, attn_gain),
                (wd_ref, wd),
                (wb_ref, wb),
                (rate_ref, rate),
                (bias_ref, bias),
                (og_ref, out_gain),
                (ffn_ref, ffn_gain),
                (routes_ref, routes),
                (weights_ref, weights),
            )
        )
    ]
    weight = [(src, wbuf.at[n]) for n, src in enumerate((wq, wk, wv, wz))] + [(w_out, wo)]

    def load_start(n):
        pltpu.make_async_copy(*weight[n], w_sem.at[n]).start()

    def load_wait(n):
        pltpu.make_async_copy(*weight[n], w_sem.at[n]).wait()

    experts = [
        pltpu.make_async_copy(src.at[0], dst.at[t], x_sem.at[n])
        for n, (src, dst) in enumerate(((w_gate, wg), (w_up, wu), (w_down, wdn)))
    ]
    push = [
        pltpu.make_async_remote_copy(
            src_ref=dst.at[t],
            dst_ref=dst.at[t],
            send_sem=push_sem.at[0, n],
            recv_sem=push_sem.at[1, n],
            device_id=partner,
            device_id_type=mesh_ids,
        )
        for n, dst in enumerate((wg, wu, wdn))
    ]
    for copy in small:
        copy.start()
    load_start(0)
    load_start(1)
    for copy in small:
        copy.wait()
    load_start(2)

    normed = rms_scale(tokens[...].astype(F32), attn_gain[...]).astype(BF16)

    def rounded(weight):
        return jnp.dot(normed, weight, preferred_element_type=F32).astype(BF16).astype(F32)

    xa = nt_dot(normed, wd[...]).astype(BF16).astype(F32) + bias[...]
    fade = jnp.exp(-rate[...] * (jnp.maximum(xa, 0.0) + jnp.log1p(jnp.exp(-jnp.abs(xa)))))
    beta = jax.nn.sigmoid(nt_dot(normed, wb[...]).astype(BF16).astype(F32))
    for h in range(heads):
        fades[:, h, :] = jnp.broadcast_to(fade[:, h : h + 1], (seqs, dim))
        betas[:, h, :] = jnp.broadcast_to(beta[:, h : h + 1], (seqs, dim))

    eye = iota((seqs, seqs), 1) == iota((seqs, seqs), 0)

    def column(row):
        return jnp.sum(jnp.where(eye, row, 0.0), axis=1, keepdims=True)

    lower = (iota((seqs, seqs), 1) < iota((seqs, seqs), 0)).astype(BF16)
    slots = n_ep * cap
    taken = jnp.zeros((1, n_ep), F32)
    found = []
    mine = jnp.zeros((seqs, slots), F32)
    for j in range(top):
        route = column(routes[j : j + 1, :].astype(F32)).astype(jnp.int32)
        hot = (iota((seqs, n_ep), 1) == route).astype(F32)
        before = jnp.dot(lower, hot.astype(BF16), preferred_element_type=F32) + taken
        slot = jnp.sum(before * hot, axis=1, keepdims=True).astype(jnp.int32)
        taken = taken + jnp.sum(hot, axis=0, keepdims=True)
        place = route * cap + slot + jnp.where(slot < shares[0], 0, slots - shares[0])
        found.append((iota((seqs, n_tp * slots), 1) == place).astype(F32))
        mine = mine + (iota((seqs, slots), 1) + t * slots == place).astype(F32)
    spread[...] = mine.T.astype(BF16)
    picks[...] = jnp.concatenate(found, axis=0).astype(BF16)

    load_wait(0)
    for c in range(chunks // 3):
        in_copy(c).start()
    raw_q = rounded(wbuf[0])
    load_wait(1)
    for c in range(chunks // 3, 2 * chunks // 3):
        in_copy(c).start()
    raw_k = rounded(wbuf[1])
    for h in range(heads):
        span = slice(h * dim, (h + 1) * dim)
        query = unit_rows(silu(raw_q[:, span])) * dim ** (-0.5)
        key = unit_rows(silu(raw_k[:, span]))
        kq[:, h, :] = key
        turned[h] = key.T
        kq[:, heads + h, :] = query
        dots[:, h, :] = jnp.broadcast_to(jnp.sum(key * query, axis=-1, keepdims=True), (seqs, dim))
    load_wait(2)
    load_start(3)
    for c in range(2 * chunks // 3, chunks):
        in_copy(c).start()
    value = silu(rounded(wbuf[2]))
    for h in range(heads):
        vals[:, h, :] = value[:, h * dim : (h + 1) * dim]

    def hits_of(c):
        in_copy(c).wait()
        hits = []
        for s in range(c * step, (c + 1) * step):
            lhs = kq[s].astype(BF16)
            hits.append([jnp.dot(lhs, ns[s, h].astype(BF16), preferred_element_type=F32) for h in range(heads)])
        return hits

    def update(c, hits):
        for i in range(step):
            s = c * step + i
            fs, bs, vs, ds = fades[s], betas[s], vals[s], dots[s]
            for h in range(heads):
                hit = hits[i][h]
                f = fs[h : h + 1]
                written = bs[h : h + 1] * (vs[h : h + 1] - f * hit[h : h + 1])
                kc = jnp.broadcast_to(turned[h, :, s : s + 1], (dim, dim))
                ns[s, h] = f * ns[s, h] + kc * written
                reads[s, pl.ds(h, 1)] = f * hit[heads + h : heads + h + 1] + written * ds[h : h + 1]

    before = None
    zc = max(chunks - 2, 0)
    for c in range(chunks):
        hits = hits_of(c)
        if c == min(1, chunks - 1):
            load_start(4)
        if c == chunks - 1:
            experts[0].start()
        if c == zc:
            load_wait(3)
            zbuf[...] = silu(rounded(wbuf[3]))
        if before is not None:
            update(c - 1, before)
        before = hits
    update(chunks - 1, before)
    for copy in experts[1:]:
        copy.start()
    mixed = []
    for h in range(heads):
        span = slice(h * dim, (h + 1) * dim)
        mixed.append((rms_scale(reads[:, h, :], out_gain[...]) * zbuf[:, span]).astype(BF16))
    load_wait(4)
    part_out[...] = jnp.dot(jnp.concatenate(mixed, axis=1), wo[...], preferred_element_type=F32).astype(BF16)
    pl.semaphore_wait(barrier, n_ep)

    swap = pltpu.make_async_remote_copy(
        src_ref=part_out,
        dst_ref=part_in,
        send_sem=part_sem.at[0],
        recv_sem=part_sem.at[1],
        device_id=partner,
        device_id_type=mesh_ids,
    )
    swap.start()
    experts[0].wait()
    push[0].start()
    swap.wait_recv()
    rows = tokens[...].astype(F32) + (part_out[...].astype(F32) + part_in[...].astype(F32))
    resid[...] = rows
    moe = rms_scale(rows, ffn_gain[...]).astype(BF16)
    going = jnp.dot(spread[...], moe, preferred_element_type=F32)
    disp[...] = going.reshape(n_ep, cap, width).astype(BF16)

    def go(n, p):
        return pltpu.make_async_remote_copy(
            src_ref=disp.at[p, pl.ds(0, n)],
            dst_ref=arrived.at[rank, pl.ds(0, n)],
            send_sem=go_sem.at[groups],
            recv_sem=go_sem.at[mine_group],
            device_id={"ep": p, "tp": t},
            device_id_type=mesh_ids,
        )

    def all_go(n, count, which):
        block = arrived.at[pl.ds(0, count), pl.ds(0, n)]
        return pltpu.make_async_copy(block, block, go_sem.at[which])

    def back(n, c, k):
        return pltpu.make_async_remote_copy(
            src_ref=ret_out.at[c, k, pl.ds(0, n)],
            dst_ref=ret_in.at[t, e, pl.ds(0, n)],
            send_sem=back_sem.at[0],
            recv_sem=back_recv.at[t],
            device_id={"ep": order[k], "tp": c},
            device_id_type=mesh_ids,
        )

    def all_back(n, c, count, sem):
        block = ret_in.at[c, pl.ds(0, count), pl.ds(0, n)]
        return pltpu.make_async_copy(block, block, sem)

    for c, n in enumerate(shares):
        if n:

            @pl.when(t == c)
            def _(n=n):
                for i in range(1, n_ep):
                    go(n, peer(i)).start()

    arrived[rank] = disp[e]
    for n in (1, 2):
        experts[n].wait()
        push[n].start()
    for g in range(groups):
        low, high = bounds[g], bounds[g + 1]
        size = high - low
        span = pl.ds(low, size)
        for c, n in enumerate(shares):
            if n:

                @pl.when((t == c) & (mine_group == g))
                def _(n=n, g=g, size=size):
                    if size > 1:
                        all_go(n, size - 1, g).wait()

                @pl.when((t == c) & (mine_group != g))
                def _(n=n, g=g, size=size):
                    all_go(n, size, g).wait()

        got = arrived[span].astype(F32).reshape(size * cap, width).astype(BF16)
        if g == 0:
            push[0].wait_recv()
        gates = [jnp.dot(got, wg[h], preferred_element_type=F32) for h in range(n_tp)]
        if g == 0:
            push[1].wait_recv()
        ups = [jnp.dot(got, wu[h], preferred_element_type=F32) for h in range(n_tp)]
        hidden = [(silu(gates[h]) * ups[h]).astype(BF16) for h in range(n_tp)]
        if g == 0:
            push[2].wait_recv()
        for d in range(n_tp):
            term = None
            for h in range(n_tp):
                piece = jnp.dot(hidden[h], wdn[h, :, d * cols : (d + 1) * cols], preferred_element_type=F32)
                term = piece if term is None else term + piece
            ret_out[d, span] = term.reshape(size, cap, cols).astype(BF16)
            for c, n in enumerate(shares):
                if n:

                    @pl.when(t == c)
                    def _(n=n, c=c, d=d, low=low, high=high):
                        for k in range(low, high):
                            if d != c:
                                back(n, d, k).start()
                            else:

                                @pl.when(e != order[k])
                                def _(k=k):
                                    back(n, d, k).start()

    ret_in[t, e] = ret_out[t, rank]
    total = resid[:, pl.ds(pl.multiple_of(t * cols, 128), cols)]
    scale = [column(weights[j : j + 1, :]) for j in range(top)]
    for c, n in enumerate(shares):
        if n:
            for d in range(n_tp):

                @pl.when(t == d)
                def _(n=n, c=c, d=d):
                    all_back(n, c, n_ep - (c == d), back_recv.at[c]).wait()

    kept = [(iota((n_ep, cap, cols), 1) < n) for n in shares]
    returned = [
        jnp.where(kept[c], ret_in[c].astype(F32), 0.0).reshape(slots, cols).astype(BF16) for c in range(n_tp)
    ]
    combined = jnp.dot(picks[...], jnp.concatenate(returned, axis=0), preferred_element_type=F32)
    for j in range(top):
        total = total + combined[j * seqs : (j + 1) * seqs] * scale[j]
    out[...] = total.astype(BF16)

    for copy in (swap, *push):
        copy.wait_send()
    for c, n in enumerate(shares):
        if n:

            @pl.when(t == c)
            def _(n=n):
                all_go(n, n_ep - 1, groups).wait()
                for d in range(n_tp):
                    all_back(n, d, n_ep - 1 + d, back_sem.at[0]).wait()


def flush_kernel(step, out_ref, ns_ref, out, ns, sem):
    copies = [pltpu.make_async_copy(out_ref, out, sem.at[0])]
    for s in range(0, ns.shape[0], step):
        rows = pl.ds(s, step)
        copies.append(pltpu.make_async_copy(ns_ref.at[rows], ns.at[rows], sem.at[1]))
    for copy in copies:
        copy.start()
    copies[0].wait()
    pltpu.make_async_copy(ns_ref, ns, sem.at[1]).wait()


def per_device(
    n_ep,
    n_tp,
    order,
    tokens,
    attn_gain,
    w_query,
    w_key,
    w_value,
    w_zgate,
    w_decay,
    w_beta,
    decay_rate,
    decay_bias,
    state,
    out_gain,
    w_out,
    ffn_gain,
    expert_gate,
    expert_up,
    expert_down,
    routes,
    route_weight,
):
    seqs, width = tokens.shape
    heads, dim = state.shape[1], state.shape[2]
    top = routes.shape[1]
    inner = heads * dim
    step = 4 if seqs % 4 == 0 else 1
    chunks = seqs // step
    live = max(2, 2 * seqs * top // n_ep)
    most = 2 * -(-live // 4)
    shares = (live - most, most)
    cap = -(-most // 8) * 8
    bounds = sorted({0, n_ep, *(n_ep * share // 16 for share in CUTS)})
    groups = len(bounds) - 1
    cols = width // n_tp
    ff = expert_gate.shape[2]
    slots = n_ep * cap
    vmem = pltpu.VMEM
    dma = pltpu.SemaphoreType.DMA
    layer_out, new_state = pl.pallas_call(
        functools.partial(layer_kernel, n_ep, n_tp, top, cap, shares, step, order, bounds),
        out_shape=(vmem((seqs, cols), BF16), vmem(state.shape, F32)),
        in_specs=[HBM] * 19,
        out_specs=(VMEM, VMEM),
        scratch_shapes=[
            vmem((seqs, width), BF16),
            vmem((1, width), F32),
            vmem((heads, width), BF16),
            vmem((heads, width), BF16),
            vmem((1, heads), F32),
            vmem((1, heads), F32),
            vmem((1, dim), F32),
            vmem((1, width), F32),
            vmem((top, seqs), jnp.int32),
            vmem((top, seqs), F32),
            vmem((4, width, inner), BF16),
            vmem((inner, width), BF16),
            vmem((n_tp, width, ff), BF16),
            vmem((n_tp, width, ff), BF16),
            vmem((n_tp, ff, width), BF16),
            vmem((seqs, 2 * heads, dim), F32),
            vmem((seqs, heads, dim), F32),
            vmem((seqs, inner), F32),
            vmem((seqs, heads, dim), F32),
            vmem((seqs, heads, dim), F32),
            vmem((seqs, heads, dim), F32),
            vmem((heads, dim, seqs), F32),
            vmem((seqs, heads, dim), F32),
            vmem((slots, seqs), BF16),
            vmem((top * seqs, n_tp * slots), BF16),
            vmem((seqs, width), BF16),
            vmem((seqs, width), BF16),
            vmem((seqs, width), F32),
            vmem((n_ep, cap, width), BF16),
            vmem((n_ep, cap, width), BF16),
            vmem((n_tp, n_ep, cap, cols), BF16),
            vmem((n_tp, n_ep, cap, cols), BF16),
            dma((10,)),
            dma((5,)),
            dma((chunks,)),
            dma((3,)),
            dma((2,)),
            dma((2, 3)),
            dma((groups + 1,)),
            dma((1,)),
            dma((n_tp,)),
        ],
        compiler_params=pltpu.CompilerParams(
            collective_id=0, has_side_effects=True, vmem_limit_bytes=VMEM_LIMIT
        ),
        name="layer",
    )(
        tokens,
        attn_gain.reshape(1, width),
        w_decay.T,
        w_beta.T,
        decay_rate.reshape(1, heads),
        decay_bias.reshape(1, heads),
        out_gain.reshape(1, dim),
        ffn_gain.reshape(1, width),
        routes.T,
        route_weight.T,
        w_query,
        w_key,
        w_value,
        w_zgate,
        state,
        w_out,
        expert_gate,
        expert_up,
        expert_down,
    )
    return pl.pallas_call(
        functools.partial(flush_kernel, step),
        out_shape=(jax.ShapeDtypeStruct((seqs, cols), BF16), jax.ShapeDtypeStruct(state.shape, F32)),
        in_specs=[VMEM, VMEM],
        out_specs=(HBM, HBM),
        scratch_shapes=[dma((2,))],
        compiler_params=pltpu.CompilerParams(vmem_limit_bytes=2**20),
        name="flush",
    )(
        pltpu.with_memory_space_constraint(layer_out, pltpu.VMEM),
        pltpu.with_memory_space_constraint(new_state, pltpu.VMEM),
    )


def solution(mesh):
    in_specs = (
        P("ep", None),
        P(),
        P(None, "tp"),
        P(None, "tp"),
        P(None, "tp"),
        P(None, "tp"),
        P(None, "tp"),
        P(None, "tp"),
        P("tp"),
        P("tp"),
        P("ep", "tp", None, None),
        P(),
        P("tp", None),
        P(),
        P("ep", None, "tp"),
        P("ep", None, "tp"),
        P("ep", "tp", None),
        P("ep", None),
        P("ep", None),
    )
    out_specs = (P("ep", "tp"), P("ep", "tp", None, None))
    n_ep, n_tp = mesh.shape["ep"], mesh.shape["tp"]
    chips = mesh.devices.reshape(n_ep, n_tp)[:, 0]
    order = sorted(range(n_ep), key=lambda p: sum(getattr(chips[p], "coords", (p,))))
    body = functools.partial(per_device, n_ep, n_tp, order)
    return jax.shard_map(body, mesh=mesh, in_specs=in_specs, out_specs=out_specs, check_vma=False)
```
